32 devices in a mesh: sp: 8 (over z, y), tp: 4 (over x, core).
Axes of the slice: x: 2, y: 2, z: 4, core: 2. Of those that a mesh axis runs over, the one named last changes fastest.
Arguments:
- hidden_state: bfloat16 [1024, 2048], P('sp'), may hold values from -6 to 6
- out_grad: bfloat16 [1024, 2048], P('sp'), may hold values from -8 to 8
- routes: int32 [1024, 2], P('sp'), may hold values from 0 to 3, all different within a row; in each aligned block of 128 rows (0 to 127, 128 to 255, ...) at most 96 rows name the same one
- route_weights: float32 [1024, 2], P('sp'), may hold values from 0.25 to 1
- w_gate: bfloat16 [8, 2048, 1792], P('sp', None, 'tp'), may hold values from -0.125 to 0.125
- w_up: bfloat16 [8, 2048, 1792], P('sp', None, 'tp'), may hold values from -0.125 to 0.125
- w_down: bfloat16 [8, 1792, 2048], P('sp', 'tp'), may hold values from -0.09375 to 0.09375
- value: bfloat16 [1024, 512], P('sp', 'tp'), may hold values from -6 to 6
- gate_in: bfloat16 [1024, 512], P('sp', 'tp'), may hold values from -6 to 6
- normed: bfloat16 [1024, 512], P('sp', 'tp'), may hold values from -24 to 24
- inv_std: float32 [1024], P('sp'), may hold values from 0.5 to 2
- norm_gain: float32 [512], P('tp'), may hold values from 0.1 to 1.9
- taps: float32 [31, 512], P(None, 'tp'), may hold values from -1 to 1
- w_proj: bfloat16 [2048, 512], P(None, 'tp'), may hold values from -0.25 to 0.25
Outputs:
- w_gate_grad: bfloat16 [8, 2048, 1792], P('sp', None, 'tp')
- w_up_grad: bfloat16 [8, 2048, 1792], P('sp', None, 'tp')
- w_down_grad: bfloat16 [8, 1792, 2048], P('sp', 'tp')
- stream_grad: bfloat16 [1024, 2048], P('sp', 'tp')
- proj_grad: float32 [2048, 512], P('sp', 'tp')
- value_grad: bfloat16 [1024, 512], P('sp', 'tp')
- gate_in_grad: bfloat16 [1024, 512], P('sp', 'tp')
The draws below stay inside these ranges and needn't reach their ends.
Inputs may be any that keep to these rules, and one draw needn't show every extreme that they name: `routes`: among the choices of one device's tokens no expert is named more than 96 times, a bound that some block reaches on some device; a token's choices differ.
All inputs are finite; a program needn't handle non-finite values.
Results may differ from the reference program's by a relative error of at most 0.0057.
Values may be sent and summed in bfloat16 or wider, within the bound.
A program may use at most 128 MiB of HBM per device.

```python
import math
import jax
import jax.numpy as jnp
import numpy as np
from jax import lax

D = 2048
D_CH = 512
FF = 3584
KSIZE = 31
TOP = 2
GROUP = 2
TOK_DEV = 128
TOKENS = 1024
EXPERTS = 4
CAP = 96
N_SP = 8


def draw_normed(key, part):
    first_key, second_key, third_key = jax.random.split(key, 3)
    levels = jax.random.permutation(first_key, jnp.array([-0.7, 0.0, 0.7, 1.4], jnp.float32))
    spread = jax.random.uniform(second_key, (D_CH,), jnp.float32, -1.0, 1.0)
    channel_scale = jnp.exp(jnp.repeat(levels, D_CH // 4) + 0.3 * spread)
    base_values = jnp.clip(jax.random.normal(third_key, (TOKENS, D_CH), jnp.float32), -4.0, 4.0)
    return (base_values * channel_scale[None, :]).astype(jnp.bfloat16)


def strengthened(drawn, stream_key, source, target, parts, factor):
    owner, partner = [(jnp.arange(drawn.shape[dim]) // (drawn.shape[dim] // parts)).reshape([-1 if axis == dim else 1 for axis in range(drawn.ndim)]) for dim in (source, target)]
    chosen = jax.random.permutation(stream_key, parts)[partner]
    strong = (owner == chosen) | (owner == (partner + parts // 2) % parts)
    return jnp.where(strong, factor * drawn, drawn)


def level_of(key, shape, cuts, smallest, high):
    factor_of = 1.0
    for dim, blocks in cuts:
        heights = jax.random.uniform(jax.random.fold_in(jax.random.fold_in(key, 6), dim), (blocks,), jnp.float32, smallest / len(cuts), high / len(cuts))
        factor_of = factor_of * jnp.repeat(jnp.exp(heights), shape[dim] // blocks).reshape((-1,) + (1,) * (len(shape) - 1 - dim))
    return factor_of


def shared_out(stream_key, own, number, rows, count, top, bound, slope):
    order = jax.random.permutation(stream_key, count)
    heavy_load, common = portions_of(count, rows * top, bound, slope, True), portions_of(count, rows * top, bound, slope, False)
    places = jnp.arange(count)

    def named(tallies, offset_by):
        used = int((tallies > 0).sum())
        fixed = max(1, used // 4)
        passed = fixed + (places - fixed + offset_by * (used - fixed)) % max(1, count - fixed)
        return jnp.zeros((count,), jnp.int32).at[order[jnp.where(places < fixed, places, passed)]].set(jnp.asarray(tallies, jnp.int32))

    tallies = jnp.where(number % 4 == 0, named(heavy_load, number // 4), named(common, number - number // 4 - 1))
    mixed = jax.random.permutation(jax.random.fold_in(own, 3), count)
    giver, sink = mixed[0:count // 2 * 2:2], mixed[1:count // 2 * 2:2]
    margin = jnp.minimum(tallies[giver] - 1, bound - tallies[sink]) // 2
    margin = jnp.where((giver == order[0]) | (sink == order[0]) | (tallies[sink] == 0), 0, jnp.maximum(margin, 0))
    passed = jax.random.randint(jax.random.fold_in(own, 4), (count // 2,), 0, 1 << 20) % (margin + 1)
    tallies = tallies.at[giver].add(-passed).at[sink].add(passed)
    labels = jnp.searchsorted(jnp.cumsum(tallies), jnp.arange(rows * top), side="right").astype(jnp.int32)
    table = labels.reshape(top, rows).T
    table = table[jax.random.permutation(jax.random.fold_in(own, 1), rows)]
    offset_by = jax.random.randint(jax.random.fold_in(own, 2), (rows, 1), 0, top)
    return jnp.take_along_axis(table, (jnp.arange(top)[None, :] + offset_by) % top, axis=1)


def portions_of(count, total, reach, skew, full):
    weights = [(1 << 20) // math.isqrt(rank ** skew) + 1 for rank in range(1, count + 1)]
    largest = reach if full else min(reach, max(-(-total // count), total * weights[0] // sum(weights)))
    least = 1 if total - largest >= count - 1 else 0
    holding, surplus = [largest] + [least] * (count - 1), total - largest - least * (count - 1)
    while surplus > 0:
        free = [i for i in range(1, count) if holding[i] < largest] or [i for i in range(1, count) if holding[i] < reach]
        whole, remaining = sum([weights[i] for i in free]), surplus
        for i in free:
            extra = min(reach - holding[i], max(1, remaining * weights[i] // whole), surplus)
            holding[i] = holding[i] + extra
            surplus = surplus - extra
    return np.array(holding)


def scatter_about(key, extent, width, bound, pieces=(), kind=jnp.bfloat16):
    entries = width * jax.random.normal(key, extent, jnp.float32)
    if pieces:
        entries = entries * level_of(key, extent, pieces, -0.22, 0.18)
    return jnp.clip(entries, -bound, bound).astype(kind)


def noise_with(stream_key, extent, scale, limit, cuts, heavy, kind=jnp.bfloat16):
    values = scale * jax.random.normal(stream_key, extent, jnp.float32)
    if cuts:
        values = values * level_of(stream_key, extent, cuts, -0.22, 0.18)
    return jnp.clip(strengthened(values, jax.random.fold_in(stream_key, 3), *heavy), -limit, limit).astype(kind)


def setup_inputs(seed: int = 0) -> dict:
    seeds = jax.random.split(jax.random.key(seed), 15)
    hidden_state = scatter_about(seeds[0], (TOKENS, D), 1.0, 6.0, ((0, 8),))
    out_grad = noise_with(seeds[1], (TOKENS, D), 1.0, 8.0, ((0, 8),), (0, 1, 8, 2.0))
    routes_keys = jax.random.split(jax.random.fold_in(seeds[2], 1), TOKENS // TOK_DEV)
    routes_turns = jax.random.permutation(jax.random.fold_in(seeds[2], 3), TOKENS // TOK_DEV)
    routes = jax.vmap(lambda own, number: shared_out(jax.random.fold_in(seeds[2], 2), own, number, TOK_DEV, EXPERTS, TOP, CAP, 1))(routes_keys, routes_turns).reshape((TOKENS, TOP))
    route_weights = jnp.clip(0.25 + 0.75 * jax.random.uniform(seeds[3], (TOKENS, TOP), jnp.float32) ** level_of(seeds[3], (TOKENS, TOP), ((0, 8),), -0.2, 0.2), 0.25, 1.0)
    w_gate = scatter_about(seeds[4], (EXPERTS * GROUP, D, FF // GROUP), D ** -0.5, 0.125, ((0, 8), (2, 4)))
    w_up = scatter_about(seeds[5], (EXPERTS * GROUP, D, FF // GROUP), D ** -0.5, 0.125, ((0, 8), (2, 4)))
    w_down = scatter_about(seeds[6], (EXPERTS * GROUP, FF // GROUP, D), FF ** -0.5, 0.09375, ((0, 8), (1, 4)))
    value = scatter_about(seeds[7], (TOKENS, D_CH), 1.0, 6.0, ((0, 8), (1, 4)))
    gate_in = scatter_about(seeds[8], (TOKENS, D_CH), 1.0, 6.0, ((0, 8), (1, 4)))
    normed = draw_normed(jax.random.fold_in(seeds[14], 71), 0)
    inv_std = jnp.clip(jnp.exp(math.log(2.0) - 1.3862944 * jax.random.uniform(seeds[10], (TOKENS,), jnp.float32) ** level_of(seeds[10], (TOKENS,), ((0, 8),), -0.2, 0.2)), 0.5, 2.0)
    norm_gain = jnp.clip(1.0 + 0.18 * jax.random.normal(seeds[11], (D_CH,), jnp.float32), 0.1, 1.9)
    taps = scatter_about(seeds[12], (KSIZE, D_CH), 0.18, 1.0, ((1, 4),), jnp.float32)
    w_proj = scatter_about(seeds[13], (D, D_CH), D_CH ** -0.5, 0.25, ((1, 4),))
    return dict(hidden_state=hidden_state, out_grad=out_grad, routes=routes, route_weights=route_weights, w_gate=w_gate, w_up=w_up, w_down=w_down, value=value, gate_in=gate_in, normed=normed, inv_std=inv_std, norm_gain=norm_gain, taps=taps, w_proj=w_proj)


def expert_backward(in_rows, in_cots, gate_slice, up_slice, down_slice):
    pre_gate = jnp.dot(in_rows, gate_slice, preferred_element_type=jnp.float32)
    pre_up = jnp.dot(in_rows, up_slice, preferred_element_type=jnp.float32)
    gate_sig = jax.nn.sigmoid(pre_gate)
    silu_gate = pre_gate * gate_sig
    act_rows = (silu_gate * pre_up).astype(jnp.bfloat16)
    act_grad = lax.dot_general(in_cots, down_slice, (((1,), (1,)), ((), ())), preferred_element_type=jnp.float32)
    gate_grad = (act_grad * pre_up * gate_sig * (1.0 + pre_gate * (1.0 - gate_sig))).astype(jnp.bfloat16)
    up_grad = (act_grad * silu_gate).astype(jnp.bfloat16)
    down_grad = lax.dot_general(act_rows, in_cots, (((0,), (0,)), ((), ())), preferred_element_type=jnp.float32)
    gate_wgrad = lax.dot_general(in_rows, gate_grad, (((0,), (0,)), ((), ())), preferred_element_type=jnp.float32)
    up_wgrad = lax.dot_general(in_rows, up_grad, (((0,), (0,)), ((), ())), preferred_element_type=jnp.float32)
    row_grad = lax.dot_general(gate_grad, gate_slice, (((1,), (1,)), ((), ())), preferred_element_type=jnp.float32)
    row_grad = row_grad + lax.dot_general(up_grad, up_slice, (((1,), (1,)), ((), ())), preferred_element_type=jnp.float32)
    return gate_wgrad.astype(jnp.bfloat16), up_wgrad.astype(jnp.bfloat16), down_grad.astype(jnp.bfloat16), row_grad


def reference(hidden_state, out_grad, routes, route_weights, w_gate, w_up, w_down, value, gate_in, normed, inv_std, norm_gain, taps, w_proj):
    tokens, model_width = hidden_state.shape
    top_k = routes.shape[1]
    experts = N_SP // GROUP
    capacity = 3 * TOK_DEV * top_k // (2 * experts)
    per_dev = routes.reshape(N_SP, TOK_DEV * top_k).astype(jnp.int32)
    onehot = (per_dev[:, :, None] == jnp.arange(experts, dtype=jnp.int32)[None, None, :]).astype(jnp.int32)
    before = jnp.cumsum(onehot, axis=1) - onehot
    slot_index = jnp.sum(before * onehot, axis=2)
    source = jnp.arange(N_SP, dtype=jnp.int32)[:, None]
    slot_place = per_dev * (N_SP * capacity) + source * capacity + slot_index
    row_owner = source * TOK_DEV + jnp.arange(TOK_DEV * top_k, dtype=jnp.int32)[None, :] // top_k
    row_table = jnp.full((experts * N_SP * capacity,), tokens, jnp.int32)
    row_table = row_table.at[slot_place.reshape(-1)].set(row_owner.reshape(-1).astype(jnp.int32))
    row_table = row_table.reshape(experts, N_SP * capacity)
    row_scale = jnp.zeros((experts * N_SP * capacity,), jnp.float32)
    row_scale = row_scale.at[slot_place.reshape(-1)].set(route_weights.reshape(-1).astype(jnp.float32))
    row_scale = row_scale.reshape(experts, N_SP * capacity)
    zero_row = jnp.zeros((1, model_width), jnp.bfloat16)
    states = jnp.concatenate([hidden_state, zero_row], axis=0)
    cot_pad = jnp.concatenate([out_grad, zero_row], axis=0)

    def turn(row_total, slice_index):
        expert = (slice_index // GROUP).astype(jnp.int32)
        row_index = lax.dynamic_index_in_dim(row_table, expert, 0, False)
        scale_e = lax.dynamic_index_in_dim(row_scale, expert, 0, False)
        in_rows = jnp.take(states, row_index, axis=0)
        in_cots = (jnp.take(cot_pad, row_index, axis=0).astype(jnp.float32) * scale_e[:, None]).astype(jnp.bfloat16)
        gate_slice = lax.dynamic_index_in_dim(w_gate, slice_index, 0, False)
        up_slice = lax.dynamic_index_in_dim(w_up, slice_index, 0, False)
        down_slice = lax.dynamic_index_in_dim(w_down, slice_index, 0, False)
        gate_wgrad, up_wgrad, down_grad, row_grad = expert_backward(in_rows, in_cots, gate_slice, up_slice, down_slice)
        row_total = row_total.at[row_index].add(row_grad)
        return row_total, (gate_wgrad, up_wgrad, down_grad)

    row_total, weight_grads = lax.scan(turn, jnp.zeros((tokens + 1, model_width), jnp.float32), jnp.arange(experts * GROUP, dtype=jnp.int32))
    moe_grad = row_total[:tokens]
    stream_grad = (out_grad.astype(jnp.float32) + moe_grad).astype(jnp.bfloat16)
    proj_in = jnp.dot(stream_grad, w_proj, preferred_element_type=jnp.float32)
    saved_norm = normed.astype(jnp.float32)
    pre_act = saved_norm * norm_gain[None, :]
    act_sig = jax.nn.sigmoid(pre_act)
    silu_grad = proj_in * act_sig * (1.0 + pre_act * (1.0 - act_sig))
    norm_grad = silu_grad * norm_gain[None, :]
    mean_one = jnp.mean(norm_grad, axis=1, keepdims=True)
    mean_two = jnp.mean(norm_grad * saved_norm, axis=1, keepdims=True)
    conv_grad = inv_std[:, None] * (norm_grad - mean_one - saved_norm * mean_two)
    channels = conv_grad.shape[1]
    extended = jnp.concatenate([conv_grad, jnp.zeros((KSIZE - 1, channels), jnp.float32)], axis=0)
    glu_grad = taps[0][None, :] * extended[0:tokens]
    for tap_index in range(1, KSIZE):
        glu_grad = glu_grad + taps[tap_index][None, :] * extended[tap_index:tap_index + tokens]
    input_sig = jax.nn.sigmoid(gate_in.astype(jnp.float32))
    value_grad = (glu_grad * input_sig).astype(jnp.bfloat16)
    gate_in_grad = (glu_grad * value.astype(jnp.float32) * input_sig * (1.0 - input_sig)).astype(jnp.bfloat16)
    proj_act = (pre_act * act_sig).astype(jnp.bfloat16)
    proj_grad = lax.dot_general(stream_grad, proj_act, (((0,), (0,)), ((), ())), preferred_element_type=jnp.float32)
    return weight_grads[0], weight_grads[1], weight_grads[2], stream_grad, proj_grad, value_grad, gate_in_grad
```

```python
import functools

import jax
import jax.numpy as jnp
from jax import lax
from jax.experimental import pallas as pl
from jax.experimental.pallas import tpu as pltpu
from jax.sharding import PartitionSpec as P

GROUP = 2
PAIR = 2
MESH = pl.DeviceIdType.MESH
F32 = jnp.float32
BF16 = jnp.bfloat16


def dot_rows(a, b):
    return lax.dot_general(a, b, (((0,), (0,)), ((), ())), preferred_element_type=F32)


def dot_cols(a, b):
    return lax.dot_general(a, b, (((1,), (1,)), ((), ())), preferred_element_type=F32)


def place():
    s, t = lax.axis_index("sp"), lax.axis_index("tp")
    e, g = s // GROUP, s % GROUP
    hi, lo = t // PAIR, t % PAIR
    across = (s, (1 - hi) * PAIR + lo)
    beside = (e * GROUP + 1 - g, t)
    partner = (s, hi * PAIR + 1 - lo)
    return s, t, e, g, hi, lo, across, beside, partner


def greet(devices):
    barrier = pltpu.get_barrier_semaphore()
    for device in devices:
        pl.semaphore_signal(barrier, inc=1, device_id=device, device_id_type=MESH)
    pl.semaphore_wait(barrier, len(devices))


def remote(src, dst, send, recv, device):
    return pltpu.make_async_remote_copy(
        src_ref=src, dst_ref=dst, send_sem=send, recv_sem=recv, device_id=device, device_id_type=MESH
    )


def one_hot(rank_row, cap):
    slots = lax.broadcasted_iota(jnp.int32, (cap, rank_row.shape[1]), 0)
    return jnp.where(slots == rank_row, 1.0, 0.0)


def dispatch_kernel(experts, cap, h_ref, c_ref, rank_ref, w_ref, out_ref, pack, z_send, z_recv, g_send, g_recv):
    s, t, e, g, hi, lo, across, beside, partner = place()
    quarter = h_ref.shape[1]
    across_t = across[1]

    def loc(j, side, col):
        src = lax.rem(e + experts - j, experts)
        rows = pl.ds(pl.multiple_of((src * GROUP + side) * cap, cap), cap)
        cols = pl.ds(pl.multiple_of(col * quarter, quarter), quarter)
        return rows, cols

    z_peers = [(lax.rem(e + j, experts) * GROUP + g, t) for j in range(1, experts)]
    greet(z_peers + [across, beside, partner])
    sent = []
    own_rows, own_cols = loc(0, g, t)
    for j in list(range(1, experts)) + [0]:
        target = lax.rem(e + j, experts)
        rank_row = rank_ref[pl.ds(target, 1), :]
        hot = one_hot(rank_row, cap)
        scale = jnp.sum(hot * w_ref[pl.ds(target, 1), :], axis=1, keepdims=True)
        hot = hot.astype(BF16)
        rows = jnp.dot(hot, h_ref[...], preferred_element_type=F32).astype(BF16)
        cots = (jnp.dot(hot, c_ref[...], preferred_element_type=F32) * scale).astype(BF16)
        if j:
            pack[j, 0] = rows
            pack[j, 1] = cots
            copy = remote(
                pack.at[j], out_ref.at[:, own_rows, own_cols], z_send.at[j], z_recv.at[j], z_peers[j - 1]
            )
            copy.start()
            sent.append(copy)
        else:
            out_ref[0, own_rows, own_cols] = rows
            out_ref[1, own_rows, own_cols] = cots

    def hop(n, j, ref, device):
        return remote(ref, ref, g_send.at[j, n], g_recv.at[j, n], device)

    def send(n, j, ref, device):
        copy = hop(n, j, ref, device)
        copy.start()
        sent.append(copy)

    def full(j, side, col):
        rows, cols = loc(j, side, col)
        return out_ref.at[:, rows, cols]

    def part(k, j, side, col):
        rows, cols = loc(j, side, col)
        return out_ref.at[k, rows, cols]

    def arrived(n, j, ref):
        hop(n, j, ref, partner).wait_recv()

    def first(j):
        if j:
            block = full(j, g, t)
            remote(block, block, z_send.at[j], z_recv.at[j], partner).wait_recv()
        block = full(j, g, t)
        send(0, j, block, across)
        send(1, j, block, beside)
        send(2, j, block, partner)

    def second(j):
        arrived(0, j, full(j, g, across_t))
        send(3, j, part(0, j, g, across_t), beside)
        send(5, j, full(j, g, across_t), partner)
        arrived(1, j, full(j, 1 - g, t))
        send(4, j, part(1, j, 1 - g, t), across)
        send(6, j, full(j, 1 - g, t), partner)

    def third(j):
        arrived(3, j, part(0, j, 1 - g, across_t))
        send(7, j, part(0, j, 1 - g, across_t), partner)
        arrived(4, j, part(1, j, 1 - g, across_t))
        send(8, j, part(1, j, 1 - g, across_t), partner)

    for j in range(experts + 2):
        if j < experts:
            first(j)
        if 0 <= j - 1 < experts:
            second(j - 1)
        if 0 <= j - 2:
            third(j - 2)
    other_t = partner[1]
    far_t = (1 - hi) * PAIR + 1 - lo
    for j in range(experts):
        arrived(2, j, full(j, g, other_t))
        arrived(5, j, full(j, g, far_t))
        arrived(6, j, full(j, 1 - g, other_t))
        arrived(7, j, part(0, j, 1 - g, far_t))
        arrived(8, j, part(1, j, 1 - g, far_t))
    for copy in sent:
        copy.wait_send()


def dispatch(h_part, c_part, rank, weight, experts, cap, rows, width):
    vmem = pl.BlockSpec(memory_space=pltpu.VMEM)
    quarter = h_part.shape[1]
    return pl.pallas_call(
        functools.partial(dispatch_kernel, experts, cap),
        out_shape=jax.ShapeDtypeStruct((2, rows, width), BF16),
        in_specs=[vmem] * 4,
        out_specs=vmem,
        scratch_shapes=[
            pltpu.VMEM((experts, 2, cap, quarter), BF16),
            pltpu.SemaphoreType.DMA((experts,)),
            pltpu.SemaphoreType.DMA((experts,)),
            pltpu.SemaphoreType.DMA((experts, 9)),
            pltpu.SemaphoreType.DMA((experts, 9)),
        ],
        compiler_params=pltpu.CompilerParams(
            collective_id=0, has_side_effects=True, vmem_limit_bytes=40 * 1024 * 1024
        ),
        name="dispatch",
    )(h_part, c_part, rank, weight)


def tail_kernel(
    experts, cap, ksize,
    grad_ref, rank_ref, cot_ref, value_ref, gate_ref, normed_ref, std_ref, gain_ref, taps_ref, proj_ref,
    stream_ref, pgrad_ref, vgrad_ref, ggrad_ref,
    from_core, sums, rx_a, ry_b, relay, rx2, back, done, full, stats, ext, pg, py, pz_out, pz,
    core_send, core_recv, hop_send, hop_recv, z_send, z_recv, t_send, t_recv, p_send, p_recv, q_send, q_recv,
):
    s, t, e, g, hi, lo, across, beside, partner = place()
    sp_ways = experts * GROUP
    tok, quarter = cot_ref.shape
    half = quarter // 2
    tp_ways = stats.shape[0]
    z_peers = [(lax.rem(e + j, experts) * GROUP + g, t) for j in range(1, experts)]
    far = (s, (1 - hi) * PAIR + 1 - lo)
    before = (lax.rem(s + sp_ways - 1, sp_ways), t)
    after = (lax.rem(s + 1, sp_ways), t)
    greet(z_peers + [across, beside, partner, far, before, after])
    sent = []

    def go(copy):
        copy.start()
        sent.append(copy)

    order = list(range(1, experts)) + [0]

    def rows_of(j):
        target = lax.rem(e + j, experts)
        return pl.ds(pl.multiple_of(target * GROUP * cap, cap), GROUP * cap)

    def cols_of(col):
        return pl.ds(pl.multiple_of(col * quarter, quarter), quarter)

    def core_copy(j, h, lane):
        return remote(
            grad_ref.at[rows_of(j), cols_of(h * PAIR + lane)],
            from_core.at[j, h],
            core_send.at[j, h],
            core_recv.at[j, h],
            partner,
        )

    for j in order:
        for h in range(PAIR):
            go(core_copy(j, h, 1 - lo))

    def hop_copy(n, j, src, dst, device):
        return remote(src, dst, hop_send.at[j, n], hop_recv.at[j, n], device)

    def x_first(j):
        return hop_copy(0, j, sums.at[0, j, 1 - hi], rx_a.at[j], across)

    def y_first(j):
        return hop_copy(1, j, sums.at[1, j, :, 1 - g], ry_b.at[j], beside)

    def y_second(j):
        return hop_copy(2, j, relay.at[0, j], rx2.at[0, j], beside)

    def x_second(j):
        return hop_copy(3, j, relay.at[1, j], rx2.at[1, j], across)

    def z_copy(j):
        return remote(done.at[j], back.at[j], z_send.at[j], z_recv.at[j], z_peers[j - 1])

    def first(j):
        for h in range(PAIR):
            core_copy(j, h, lo).wait_recv()
            mine = grad_ref[rows_of(j), cols_of(h * PAIR + lo)].astype(F32)
            total = (mine + from_core[j, h].astype(F32)).astype(BF16).reshape(GROUP, cap, quarter)
            sums[0, j, h] = total[:, :, :half]
            sums[1, j, h] = total[:, :, half:]
        go(x_first(j))
        go(y_first(j))

    def second(j):
        x_first(j).wait_recv()
        relay[0, j] = (sums[0, j, hi, 1 - g].astype(F32) + rx_a[j, 1 - g].astype(F32)).astype(BF16)
        go(y_second(j))
        y_first(j).wait_recv()
        relay[1, j] = (sums[1, j, 1 - hi, g].astype(F32) + ry_b[j, 1 - hi].astype(F32)).astype(BF16)
        go(x_second(j))

    def third(j):
        y_second(j).wait_recv()
        done[j, :, :half] = (
            sums[0, j, hi, g].astype(F32) + rx_a[j, g].astype(F32) + rx2[0, j].astype(F32)
        ).astype(BF16)
        x_second(j).wait_recv()
        done[j, :, half:] = (
            sums[1, j, hi, g].astype(F32) + ry_b[j, hi].astype(F32) + rx2[1, j].astype(F32)
        ).astype(BF16)
        if j:
            go(z_copy(j))

    for i in range(experts + 2):
        if i < experts:
            first(order[i])
        if 0 <= i - 1 < experts:
            second(order[i - 1])
        if 0 <= i - 2:
            third(order[i - 2])

    gain = gain_ref[...]
    saved = normed_ref[...].astype(F32)
    pre_act = saved * gain
    act_sig = jax.nn.sigmoid(pre_act)
    slope = act_sig * (1.0 + pre_act * (1.0 - act_sig))
    proj_act = (pre_act * act_sig).astype(BF16)

    stream = cot_ref[...].astype(F32)
    for j in [0] + list(range(1, experts)):
        if j:
            z_copy(j).wait_recv()
            block = back[j]
        else:
            block = done[0]
        source = lax.rem(e + experts - j, experts)
        hot = one_hot(rank_ref[pl.ds(source, 1), :], cap).astype(BF16)
        stream = stream + dot_rows(hot, block)
    stream = stream.astype(BF16)
    stream_ref[...] = stream
    full[:, cols_of(t)] = stream

    def gather_copy(n, col, device):
        return remote(full.at[:, cols_of(col)], full.at[:, cols_of(col)], t_send.at[n], t_recv.at[n], device)

    go(gather_copy(0, t, across))
    go(gather_copy(1, t, partner))
    gather_copy(0, across[1], across).wait_recv()
    go(gather_copy(2, across[1], partner))
    gather_copy(1, partner[1], partner).wait_recv()
    gather_copy(2, far[1], partner).wait_recv()

    rows = pg.shape[2]

    def p_copy(j):
        return remote(pg.at[j, 1 - g], py.at[j], p_send.at[j], p_recv.at[j], beside)

    whole = dot_rows(full[...], proj_act)
    pall = whole.reshape(experts, GROUP, rows, whole.shape[1])
    for i in range(experts):
        pg[i] = pall[i].astype(BF16)
    for i in range(experts):
        go(p_copy(i))

    proj_in = jnp.dot(full[...], proj_ref[...], preferred_element_type=F32)
    norm_grad = proj_in * slope * gain
    one = jnp.sum(norm_grad, axis=1, keepdims=True)
    two = jnp.sum(norm_grad * saved, axis=1, keepdims=True)
    lane = lax.broadcasted_iota(jnp.int32, (tok, 128), 1)
    packed = jnp.where(lane == 0, one, jnp.where(lane == 1, two, 0.0))
    stats[t] = packed.T[:8]

    def stat_copy(n, device, owner):
        return remote(stats.at[owner], stats.at[owner], t_send.at[n], t_recv.at[n], device)

    for n, device in ((3, across), (4, far), (5, partner)):
        go(stat_copy(n, device, t))

    def q_copy(j):
        return remote(pz_out.at[j], pz.at[j], q_send.at[j], q_recv.at[j], z_peers[j - 1])

    for n, device in ((3, across), (4, far), (5, partner)):
        stat_copy(n, device, device[1]).wait_recv()
    total = stats[0]
    for i in range(1, tp_ways):
        total = total + stats[i]
    total = jnp.concatenate([total, jnp.zeros((120, tok), F32)], axis=0).T
    channels = saved.shape[1] * tp_ways
    mean_one = total[:, 0:1] / channels
    mean_two = total[:, 1:2] / channels
    conv = std_ref[...] * (norm_grad - mean_one - saved * mean_two)
    ext[pl.ds(0, tok), :] = conv

    def halo_copy():
        return remote(ext.at[pl.ds(0, 32)], ext.at[pl.ds(tok, 32)], t_send.at[6], t_recv.at[6], before)

    @pl.when(s > 0)
    def _():
        halo_copy().start()

    for i in range(experts):
        p_copy(i).wait_recv()
    for j in order:
        target = lax.rem(e + j, experts)
        piece = pg[target, g].astype(F32) + py[target].astype(F32)
        if j:
            pz_out[j] = piece.astype(BF16)
            go(q_copy(j))
        else:
            pgrad_ref[...] = piece

    @pl.when(s < sp_ways - 1)
    def _():
        halo_copy().wait_recv()

    @pl.when(s == sp_ways - 1)
    def _():
        ext[pl.ds(tok, 32), :] = jnp.zeros((32, ext.shape[1]), F32)

    glu = taps_ref[0:1, :] * ext[pl.ds(0, tok), :]
    for k in range(1, ksize):
        glu = glu + taps_ref[k : k + 1, :] * ext[pl.ds(k, tok), :]
    in_sig = jax.nn.sigmoid(gate_ref[...].astype(F32))
    vgrad_ref[...] = (glu * in_sig).astype(BF16)
    ggrad_ref[...] = (glu * value_ref[...].astype(F32) * in_sig * (1.0 - in_sig)).astype(BF16)

    total = pgrad_ref[...]
    for j in range(1, experts):
        q_copy(j).wait_recv()
        total = total + pz[j].astype(F32)
    pgrad_ref[...] = total

    @pl.when(s > 0)
    def _():
        halo_copy().wait_send()

    for copy in sent:
        copy.wait_send()


def tail(grad, rank, cot, value, gate_in, normed, std, gain, taps, w_proj, experts, cap, tp_ways):
    vmem = pl.BlockSpec(memory_space=pltpu.VMEM)
    tok, quarter = cot.shape
    width = grad.shape[1]
    ch = normed.shape[1]
    rows = width // (experts * GROUP)
    half = quarter // 2
    dma = pltpu.SemaphoreType.DMA
    assert ksize_ok(taps.shape[0])
    return pl.pallas_call(
        functools.partial(tail_kernel, experts, cap, taps.shape[0]),
        out_shape=(
            jax.ShapeDtypeStruct((tok, quarter), BF16),
            jax.ShapeDtypeStruct((rows, ch), F32),
            jax.ShapeDtypeStruct((tok, ch), BF16),
            jax.ShapeDtypeStruct((tok, ch), BF16),
        ),
        in_specs=[vmem] * 10,
        out_specs=(vmem,) * 4,
        scratch_shapes=[
            pltpu.VMEM((experts, PAIR, GROUP * cap, quarter), BF16),
            pltpu.VMEM((2, experts, PAIR, GROUP, cap, half), BF16),
            pltpu.VMEM((experts, GROUP, cap, half), BF16),
            pltpu.VMEM((experts, PAIR, cap, half), BF16),
            pltpu.VMEM((2, experts, cap, half), BF16),
            pltpu.VMEM((2, experts, cap, half), BF16),
            pltpu.VMEM((experts, cap, quarter), BF16),
            pltpu.VMEM((experts, cap, quarter), BF16),
            pltpu.VMEM((tok, width), BF16),
            pltpu.VMEM((tp_ways, 8, tok), F32),
            pltpu.VMEM((tok + 32, ch), F32),
            pltpu.VMEM((experts, GROUP, rows, ch), BF16),
            pltpu.VMEM((experts, rows, ch), BF16),
            pltpu.VMEM((experts, rows, ch), BF16),
            pltpu.VMEM((experts, rows, ch), BF16),
            dma((experts, PAIR)),
            dma((experts, PAIR)),
            dma((experts, 4)),
            dma((experts, 4)),
            dma((experts,)),
            dma((experts,)),
            dma((7,)),
            dma((7,)),
            dma((experts,)),
            dma((experts,)),
            dma((experts,)),
            dma((experts,)),
        ],
        compiler_params=pltpu.CompilerParams(
            collective_id=1, has_side_effects=True, vmem_limit_bytes=56 * 1024 * 1024
        ),
        name="tail",
    )(grad, rank, cot, value, gate_in, normed, std, gain, taps, w_proj)


def ksize_ok(taps):
    return taps - 1 <= 32


def expert_backward(in_rows, in_cots, gate_slice, up_slice, down_slice):
    pre_gate = jnp.dot(in_rows, gate_slice, preferred_element_type=F32)
    pre_up = jnp.dot(in_rows, up_slice, preferred_element_type=F32)
    gate_sig = jax.nn.sigmoid(pre_gate)
    silu_gate = pre_gate * gate_sig
    act_rows = (silu_gate * pre_up).astype(BF16)
    act_grad = dot_cols(in_cots, down_slice)
    gate_grad = (act_grad * pre_up * gate_sig * (1.0 + pre_gate * (1.0 - gate_sig))).astype(BF16)
    up_grad = (act_grad * silu_gate).astype(BF16)
    row_grad = (dot_cols(gate_grad, gate_slice) + dot_cols(up_grad, up_slice)).astype(BF16)
    down_grad = dot_rows(act_rows, in_cots).astype(BF16)
    gate_wgrad = dot_rows(in_rows, gate_grad).astype(BF16)
    up_wgrad = dot_rows(in_rows, up_grad).astype(BF16)
    return gate_wgrad, up_wgrad, down_grad, row_grad


def on_device(
    hidden_state, out_grad, routes, route_weights, w_gate, w_up, w_down,
    value, gate_in, normed, inv_std, norm_gain, taps, w_proj,
):
    tok, width = hidden_state.shape
    top_k = routes.shape[1]
    sp_ways, tp_ways = lax.axis_size("sp"), lax.axis_size("tp")
    experts = sp_ways // GROUP
    cap = 3 * tok * top_k // (2 * experts)
    cap = -(-cap // 16) * 16
    quarter = width // tp_ways
    offset = lax.axis_index("tp") * quarter
    names = routes[None, :, :] == jnp.arange(experts, dtype=jnp.int32)[:, None, None]
    named = jnp.any(names, axis=2)
    weight = jnp.sum(jnp.where(names, route_weights[None], 0.0), axis=2)
    index = jnp.arange(tok)
    earlier = (index[:, None] < index[None, :]).astype(BF16)
    rank = jnp.dot(named.astype(BF16), earlier, preferred_element_type=F32).astype(jnp.int32)
    rank = jnp.where(named, rank, -1)
    h_part = lax.dynamic_slice_in_dim(hidden_state, offset, quarter, 1)
    c_part = lax.dynamic_slice_in_dim(out_grad, offset, quarter, 1)
    got = dispatch(h_part, c_part, rank, weight, experts, cap, sp_ways * cap, width)
    gate_wgrad, up_wgrad, down_grad, row_grad = expert_backward(got[0], got[1], w_gate[0], w_up[0], w_down[0])
    stream_part, proj_grad, value_grad, gate_in_grad = tail(
        row_grad, rank, c_part, value, gate_in, normed, inv_std[:, None], norm_gain[None, :], taps, w_proj,
        experts, cap, tp_ways,
    )
    return gate_wgrad[None], up_wgrad[None], down_grad[None], stream_part, proj_grad, value_grad, gate_in_grad


def solution(mesh):
    in_specs = (
        P("sp", None), P("sp", None), P("sp", None), P("sp", None),
        P("sp", None, "tp"), P("sp", None, "tp"), P("sp", "tp", None),
        P("sp", "tp"), P("sp", "tp"), P("sp", "tp"), P("sp"), P("tp"), P(None, "tp"), P(None, "tp"),
    )
    out_specs = (
        P("sp", None, "tp"), P("sp", None, "tp"), P("sp", "tp", None),
        P("sp", "tp"), P("sp", "tp"), P("sp", "tp"), P("sp", "tp"),
    )
    return jax.shard_map(on_device, mesh=mesh, in_specs=in_specs, out_specs=out_specs, check_vma=False)
```

```python
import functools

import jax
import jax.numpy as jnp
from jax import lax
from jax.experimental import pallas as pl
from jax.experimental.pallas import tpu as pltpu
from jax.sharding import PartitionSpec as P

GROUP = 2
PAIR = 2
MESH = pl.DeviceIdType.MESH
F32 = jnp.float32
BF16 = jnp.bfloat16


def dot_rows(a, b):
    return lax.dot_general(a, b, (((0,), (0,)), ((), ())), preferred_element_type=F32)


def dot_cols(a, b):
    return lax.dot_general(a, b, (((1,), (1,)), ((), ())), preferred_element_type=F32)


def place():
    s, t = lax.axis_index("sp"), lax.axis_index("tp")
    e, g = s // GROUP, s % GROUP
    hi, lo = t // PAIR, t % PAIR
    across = (s, (1 - hi) * PAIR + lo)
    beside = (e * GROUP + 1 - g, t)
    partner = (s, hi * PAIR + 1 - lo)
    return s, t, e, g, hi, lo, across, beside, partner


def greet(devices):
    barrier = pltpu.get_barrier_semaphore()
    for device in devices:
        pl.semaphore_signal(barrier, inc=1, device_id=device, device_id_type=MESH)
    pl.semaphore_wait(barrier, len(devices))


def remote(src, dst, send, recv, device):
    return pltpu.make_async_remote_copy(
        src_ref=src, dst_ref=dst, send_sem=send, recv_sem=recv, device_id=device, device_id_type=MESH
    )


def one_hot(rank_row, cap):
    slots = lax.broadcasted_iota(jnp.int32, (cap, rank_row.shape[1]), 0)
    return jnp.where(slots == rank_row, 1.0, 0.0)


def mega_kernel(
    experts, cap, ksize,
    h_ref, cot_ref, rank_ref, w_ref, gate_hbm, up_hbm, down_hbm,
    value_ref, gate_ref, normed_ref, std_ref, gain_ref, taps_ref, proj_ref,
    gw_hbm, uw_hbm, dw_hbm, stream_ref, pgrad_ref, vgrad_ref, ggrad_ref,
    buf, pack, wg, wu, wd, act, gg, ug, grad_ref, gw, uw, dw,
    from_core, sums, rx_a, ry_b, relay, rx2, back, done, full, stats, ext, pg, py, pz_out, pz,
    w_sem, o_sem, d_send, d_recv, g_send, g_recv,
    core_send, core_recv, hop_send, hop_recv, z_send, z_recv, t_send, t_recv, p_send, p_recv, q_send, q_recv,
):
    s, t, e, g, hi, lo, across, beside, partner = place()
    sp_ways = experts * GROUP
    tok, quarter = cot_ref.shape
    half = quarter // 2
    tp_ways = stats.shape[0]
    across_t, other_t = across[1], partner[1]
    far_t = (1 - hi) * PAIR + 1 - lo
    far = (s, far_t)
    z_peers = [(lax.rem(e + j, experts) * GROUP + g, t) for j in range(1, experts)]
    before = (lax.rem(s + sp_ways - 1, sp_ways), t)
    after = (lax.rem(s + 1, sp_ways), t)
    loads = [
        pltpu.make_async_copy(src, dst, w_sem.at[n])
        for n, (src, dst) in enumerate(((gate_hbm, wg), (up_hbm, wu), (down_hbm, wd)))
    ]
    for copy in loads:
        copy.start()
    sent = []

    def go(copy):
        copy.start()
        sent.append(copy)

    def cols_of(col):
        return pl.ds(pl.multiple_of(col * quarter, quarter), quarter)

    def source_of(j):
        return lax.rem(e + experts - j, experts)

    def rows_of(j):
        return pl.ds(pl.multiple_of(source_of(j) * GROUP * cap, cap), GROUP * cap)

    def loc(j, side, col):
        return pl.ds(pl.multiple_of((source_of(j) * GROUP + side) * cap, cap), cap), cols_of(col)

    own_rows, own_cols = loc(0, g, t)

    def d_copy(j):
        return remote(pack.at[j], buf.at[:, own_rows, own_cols], d_send.at[j], d_recv.at[j], z_peers[j - 1])

    greeted = False
    for j in list(range(1, experts)) + [0]:
        target = lax.rem(e + j, experts)
        hot = one_hot(rank_ref[pl.ds(target, 1), :], cap)
        scale = jnp.sum(hot * w_ref[pl.ds(target, 1), :], axis=1, keepdims=True)
        hot = hot.astype(BF16)
        rows = jnp.dot(hot, h_ref[...], preferred_element_type=F32).astype(BF16)
        cots = (jnp.dot(hot, cot_ref[...], preferred_element_type=F32) * scale).astype(BF16)
        if j:
            pack[j, 0] = rows
            pack[j, 1] = cots
            if not greeted:
                greet(z_peers + [across, beside, partner, far, before, after])
                greeted = True
            go(d_copy(j))
        else:
            buf[0, own_rows, own_cols] = rows
            buf[1, own_rows, own_cols] = cots

    def hop(n, j, ref, device):
        return remote(ref, ref, g_send.at[j, n], g_recv.at[j, n], device)

    def both(j, side, col):
        rows, cols = loc(j, side, col)
        return buf.at[:, rows, cols]

    def one_of(k, j, side, col):
        rows, cols = loc(j, side, col)
        return buf.at[k, rows, cols]

    def arrived(n, j, ref):
        hop(n, j, ref, partner).wait_recv()

    def d_first(j):
        block = both(j, g, t)
        if j:
            remote(block, block, d_send.at[j], d_recv.at[j], partner).wait_recv()
        go(hop(0, j, block, across))
        go(hop(1, j, block, beside))
        go(hop(2, j, block, partner))

    def d_second(j):
        arrived(0, j, both(j, g, across_t))
        go(hop(3, j, one_of(0, j, g, across_t), beside))
        go(hop(5, j, both(j, g, across_t), partner))
        arrived(1, j, both(j, 1 - g, t))
        go(hop(4, j, one_of(1, j, 1 - g, t), across))
        go(hop(6, j, both(j, 1 - g, t), partner))

    def d_third(j):
        arrived(3, j, one_of(0, j, 1 - g, across_t))
        go(hop(7, j, one_of(0, j, 1 - g, across_t), partner))
        arrived(4, j, one_of(1, j, 1 - g, across_t))
        go(hop(8, j, one_of(1, j, 1 - g, across_t), partner))

    def d_last(j):
        arrived(2, j, both(j, g, other_t))
        arrived(5, j, both(j, g, far_t))
        arrived(6, j, both(j, 1 - g, other_t))
        arrived(7, j, one_of(0, j, 1 - g, far_t))
        arrived(8, j, one_of(1, j, 1 - g, far_t))

    def compute(j):
        rows = rows_of(j)
        in_rows = buf[0, rows, :]
        in_cots = buf[1, rows, :]
        pre_gate = jnp.dot(in_rows, wg[...], preferred_element_type=F32)
        pre_up = jnp.dot(in_rows, wu[...], preferred_element_type=F32)
        gate_sig = jax.nn.sigmoid(pre_gate)
        silu_gate = pre_gate * gate_sig
        act_grad = dot_cols(in_cots, wd[...])
        gate_grad = (act_grad * pre_up * gate_sig * (1.0 + pre_gate * (1.0 - gate_sig))).astype(BF16)
        up_grad = (act_grad * silu_gate).astype(BF16)
        act[rows, :] = (silu_gate * pre_up).astype(BF16)
        gg[rows, :] = gate_grad
        ug[rows, :] = up_grad
        grad_ref[rows, :] = (dot_cols(gate_grad, wg[...]) + dot_cols(up_grad, wu[...])).astype(BF16)

    width = full.shape[1]
    piece = 256
    per_item = width // piece // 4

    def weight_item(which, n):
        @pl.loop(n * per_item, (n + 1) * per_item)
        def _(i):
            cols = pl.ds(pl.multiple_of(i * piece, piece), piece)
            if which == 0:
                gw[cols, :] = dot_rows(buf[0, :, cols], gg[...]).astype(BF16)
            elif which == 1:
                uw[cols, :] = dot_rows(buf[0, :, cols], ug[...]).astype(BF16)
            else:
                dw[:, cols] = dot_rows(act[...], buf[1, :, cols]).astype(BF16)

    stores = [
        pltpu.make_async_copy(src, dst, o_sem.at[n])
        for n, (src, dst) in enumerate(((gw, gw_hbm), (uw, uw_hbm), (dw, dw_hbm)))
    ]
    items = [(which, n) for which in range(3) for n in range(4)]

    def fill(count=1):
        for _ in range(count):
            if items:
                which, n = items.pop(0)
                weight_item(which, n)
                if n == 3:
                    stores[which].start()

    def core_copy(j, h, lane):
        return remote(
            grad_ref.at[rows_of(j), cols_of(h * PAIR + lane)],
            from_core.at[j, h], core_send.at[j, h], core_recv.at[j, h], partner,
        )

    def hop_copy(n, j, src, dst, device):
        return remote(src, dst, hop_send.at[j, n], hop_recv.at[j, n], device)

    def x_first(j):
        return hop_copy(0, j, sums.at[0, j, 1 - hi], rx_a.at[j], across)

    def y_first(j):
        return hop_copy(1, j, sums.at[1, j, :, 1 - g], ry_b.at[j], beside)

    def y_second(j):
        return hop_copy(2, j, relay.at[0, j], rx2.at[0, j], beside)

    def x_second(j):
        return hop_copy(3, j, relay.at[1, j], rx2.at[1, j], across)

    def z_copy(j):
        return remote(done.at[j], back.at[j], z_send.at[j], z_recv.at[j], (source_of(j) * GROUP + g, t))

    def first(j):
        for h in range(PAIR):
            core_copy(j, h, lo).wait_recv()
            mine = grad_ref[rows_of(j), cols_of(h * PAIR + lo)].astype(F32)
            total = (mine + from_core[j, h].astype(F32)).astype(BF16).reshape(GROUP, cap, quarter)
            sums[0, j, h] = total[:, :, :half]
            sums[1, j, h] = total[:, :, half:]
        go(x_first(j))
        go(y_first(j))

    def second(j):
        x_first(j).wait_recv()
        relay[0, j] = (sums[0, j, hi, 1 - g].astype(F32) + rx_a[j, 1 - g].astype(F32)).astype(BF16)
        go(y_second(j))
        y_first(j).wait_recv()
        relay[1, j] = (sums[1, j, 1 - hi, g].astype(F32) + ry_b[j, 1 - hi].astype(F32)).astype(BF16)
        go(x_second(j))

    def third(j):
        y_second(j).wait_recv()
        done[j, :, :half] = (
            sums[0, j, hi, g].astype(F32) + rx_a[j, g].astype(F32) + rx2[0, j].astype(F32)
        ).astype(BF16)
        x_second(j).wait_recv()
        done[j, :, half:] = (
            sums[1, j, hi, g].astype(F32) + ry_b[j, hi].astype(F32) + rx2[1, j].astype(F32)
        ).astype(BF16)
        if j:
            go(z_copy(j))

    step = max(1, experts // 4)
    chunks = [list(range(c, min(c + step, experts))) for c in range(0, experts, step)]

    def returns(c, fills):
        for stage, lag in ((first, 1), (second, 2), (third, 3)):
            if 0 <= c - lag < len(chunks):
                for j in chunks[c - lag]:
                    stage(j)
                fill(fills)

    for i in range(experts + 3):
        if i < experts:
            d_first(i)
        if 0 <= i - 1 < experts:
            d_second(i - 1)
        if 0 <= i - 2 < experts:
            d_third(i - 2)
        j = i - 3
        if j >= 0:
            if j == 0:
                for copy in loads:
                    copy.wait()
            d_last(j)
            if j % step == step - 1 or j == experts - 1:
                c = j // step
                if len(chunks[c]) == 1:
                    compute(j)
                else:
                    pl.loop(chunks[c][0], chunks[c][-1] + 1)(compute)
                for k in chunks[c]:
                    for h in range(PAIR):
                        go(core_copy(k, h, 1 - lo))
                returns(c, 1 if c == len(chunks) - 1 else 0)
    for c in range(len(chunks), len(chunks) + 3):
        returns(c, 1)
    fill(len(items))

    gain = gain_ref[...]
    saved = normed_ref[...].astype(F32)
    pre_act = saved * gain
    act_sig = jax.nn.sigmoid(pre_act)
    slope = act_sig * (1.0 + pre_act * (1.0 - act_sig))
    proj_act = (pre_act * act_sig).astype(BF16)

    stream = cot_ref[...].astype(F32)
    for j in [0] + list(range(1, experts)):
        if j:
            z_copy(j).wait_recv()
            block = back[j]
        else:
            block = done[0]
        source = lax.rem(e + j, experts)
        hot = one_hot(rank_ref[pl.ds(source, 1), :], cap).astype(BF16)
        stream = stream + dot_rows(hot, block)
    stream = stream.astype(BF16)
    stream_ref[...] = stream
    full[:, cols_of(t)] = stream

    def gather_copy(n, col, device):
        return remote(full.at[:, cols_of(col)], full.at[:, cols_of(col)], t_send.at[n], t_recv.at[n], device)

    go(gather_copy(0, t, across))
    go(gather_copy(1, t, partner))
    gather_copy(0, across[1], across).wait_recv()
    go(gather_copy(2, across[1], partner))
    gather_copy(1, partner[1], partner).wait_recv()
    gather_copy(2, far[1], partner).wait_recv()

    rows = pg.shape[2]

    def p_copy(j):
        return remote(pg.at[j, 1 - g], py.at[j], p_send.at[j], p_recv.at[j], beside)

    whole = dot_rows(full[...], proj_act)
    pall = whole.reshape(experts, GROUP, rows, whole.shape[1])
    for i in range(experts):
        pg[i] = pall[i].astype(BF16)
    for i in range(experts):
        go(p_copy(i))

    proj_in = jnp.dot(full[...], proj_ref[...], preferred_element_type=F32)
    norm_grad = proj_in * slope * gain
    one = jnp.sum(norm_grad, axis=1, keepdims=True)
    two = jnp.sum(norm_grad * saved, axis=1, keepdims=True)
    lane = lax.broadcasted_iota(jnp.int32, (tok, 128), 1)
    packed = jnp.where(lane == 0, one, jnp.where(lane == 1, two, 0.0))
    stats[t] = packed.T[:8]

    def stat_copy(n, device, owner):
        return remote(stats.at[owner], stats.at[owner], t_send.at[n], t_recv.at[n], device)

    for n, device in ((3, across), (4, far), (5, partner)):
        go(stat_copy(n, device, t))

    def q_copy(j):
        return remote(pz_out.at[j], pz.at[j], q_send.at[j], q_recv.at[j], z_peers[j - 1])

    for n, device in ((3, across), (4, far), (5, partner)):
        stat_copy(n, device, device[1]).wait_recv()
    total = stats[0]
    for i in range(1, tp_ways):
        total = total + stats[i]
    total = jnp.concatenate([total, jnp.zeros((120, tok), F32)], axis=0).T
    channels = saved.shape[1] * tp_ways
    mean_one = total[:, 0:1] / channels
    mean_two = total[:, 1:2] / channels
    conv = std_ref[...] * (norm_grad - mean_one - saved * mean_two)
    ext[pl.ds(0, tok), :] = conv

    def halo_copy():
        return remote(ext.at[pl.ds(0, 32)], ext.at[pl.ds(tok, 32)], t_send.at[6], t_recv.at[6], before)

    @pl.when(s > 0)
    def _():
        halo_copy().start()

    for i in range(experts):
        p_copy(i).wait_recv()
    for j in list(range(1, experts)) + [0]:
        target = lax.rem(e + j, experts)
        piece = pg[target, g].astype(F32) + py[target].astype(F32)
        if j:
            pz_out[j] = piece.astype(BF16)
            go(q_copy(j))
        else:
            pgrad_ref[...] = piece

    @pl.when(s < sp_ways - 1)
    def _():
        halo_copy().wait_recv()

    @pl.when(s == sp_ways - 1)
    def _():
        ext[pl.ds(tok, 32), :] = jnp.zeros((32, ext.shape[1]), F32)

    glu = taps_ref[0:1, :] * ext[pl.ds(0, tok), :]
    for k in range(1, ksize):
        glu = glu + taps_ref[k : k + 1, :] * ext[pl.ds(k, tok), :]
    in_sig = jax.nn.sigmoid(gate_ref[...].astype(F32))
    vgrad_ref[...] = (glu * in_sig).astype(BF16)
    ggrad_ref[...] = (glu * value_ref[...].astype(F32) * in_sig * (1.0 - in_sig)).astype(BF16)

    total = pgrad_ref[...]
    for j in range(1, experts):
        q_copy(j).wait_recv()
        total = total + pz[j].astype(F32)
    pgrad_ref[...] = total

    @pl.when(s > 0)
    def _():
        halo_copy().wait_send()

    for copy in sent:
        copy.wait_send()
    for copy in stores:
        copy.wait()


def mega(h_part, rank, weight, w_gate, w_up, w_down, cot, value, gate_in, normed, std, gain, taps, w_proj, experts, cap, tp_ways):
    vmem = pl.BlockSpec(memory_space=pltpu.VMEM)
    hbm = pl.BlockSpec(memory_space=pl.ANY)
    tok, quarter = cot.shape
    width, hidden = w_gate.shape
    total = experts * GROUP * cap
    ch = normed.shape[1]
    rows = width // (experts * GROUP)
    half = quarter // 2
    dma = pltpu.SemaphoreType.DMA
    assert taps.shape[0] - 1 <= 32
    return pl.pallas_call(
        functools.partial(mega_kernel, experts, cap, taps.shape[0]),
        out_shape=(
            jax.ShapeDtypeStruct((width, hidden), BF16),
            jax.ShapeDtypeStruct((width, hidden), BF16),
            jax.ShapeDtypeStruct((hidden, width), BF16),
            jax.ShapeDtypeStruct((tok, quarter), BF16),
            jax.ShapeDtypeStruct((rows, ch), F32),
            jax.ShapeDtypeStruct((tok, ch), BF16),
            jax.ShapeDtypeStruct((tok, ch), BF16),
        ),
        in_specs=[vmem] * 4 + [hbm] * 3 + [vmem] * 7,
        out_specs=(hbm,) * 3 + (vmem,) * 4,
        scratch_shapes=[
            pltpu.VMEM((2, total, width), BF16),
            pltpu.VMEM((experts, 2, cap, quarter), BF16),
            pltpu.VMEM((width, hidden), BF16),
            pltpu.VMEM((width, hidden), BF16),
            pltpu.VMEM((hidden, width), BF16),
            pltpu.VMEM((total, hidden), BF16),
            pltpu.VMEM((total, hidden), BF16),
            pltpu.VMEM((total, hidden), BF16),
            pltpu.VMEM((total, width), BF16),
            pltpu.VMEM((width, hidden), BF16),
            pltpu.VMEM((width, hidden), BF16),
            pltpu.VMEM((hidden, width), BF16),
            pltpu.VMEM((experts, PAIR, GROUP * cap, quarter), BF16),
            pltpu.VMEM((2, experts, PAIR, GROUP, cap, half), BF16),
            pltpu.VMEM((experts, GROUP, cap, half), BF16),
            pltpu.VMEM((experts, PAIR, cap, half), BF16),
            pltpu.VMEM((2, experts, cap, half), BF16),
            pltpu.VMEM((2, experts, cap, half), BF16),
            pltpu.VMEM((experts, cap, quarter), BF16),
            pltpu.VMEM((experts, cap, quarter), BF16),
            pltpu.VMEM((tok, width), BF16),
            pltpu.VMEM((tp_ways, 8, tok), F32),
            pltpu.VMEM((tok + 32, ch), F32),
            pltpu.VMEM((experts, GROUP, rows, ch), BF16),
            pltpu.VMEM((experts, rows, ch), BF16),
            pltpu.VMEM((experts, rows, ch), BF16),
            pltpu.VMEM((experts, rows, ch), BF16),
            dma((3,)),
            dma((3,)),
            dma((experts,)),
            dma((experts,)),
            dma((experts, 9)),
            dma((experts, 9)),
            dma((experts, PAIR)),
            dma((experts, PAIR)),
            dma((experts, 4)),
            dma((experts, 4)),
            dma((experts,)),
            dma((experts,)),
            dma((7,)),
            dma((7,)),
            dma((experts,)),
            dma((experts,)),
            dma((experts,)),
            dma((experts,)),
        ],
        compiler_params=pltpu.CompilerParams(
            collective_id=0, has_side_effects=True, vmem_limit_bytes=56 * 1024 * 1024
        ),
        name="mega",
    )(h_part, cot, rank, weight, w_gate, w_up, w_down, value, gate_in, normed, std, gain, taps, w_proj)


def on_device(
    hidden_state, out_grad, routes, route_weights, w_gate, w_up, w_down,
    value, gate_in, normed, inv_std, norm_gain, taps, w_proj,
):
    tok, width = hidden_state.shape
    top_k = routes.shape[1]
    sp_ways, tp_ways = lax.axis_size("sp"), lax.axis_size("tp")
    experts = sp_ways // GROUP
    cap = 3 * tok * top_k // (2 * experts)
    cap = -(-cap // 16) * 16
    quarter = width // tp_ways
    offset = lax.axis_index("tp") * quarter
    names = routes[None, :, :] == jnp.arange(experts, dtype=jnp.int32)[:, None, None]
    named = jnp.any(names, axis=2)
    weight = jnp.sum(jnp.where(names, route_weights[None], 0.0), axis=2)
    index = jnp.arange(tok)
    earlier = (index[:, None] < index[None, :]).astype(BF16)
    rank = jnp.dot(named.astype(BF16), earlier, preferred_element_type=F32).astype(jnp.int32)
    rank = jnp.where(named, rank, -1)
    h_part = lax.dynamic_slice_in_dim(hidden_state, offset, quarter, 1)
    c_part = lax.dynamic_slice_in_dim(out_grad, offset, quarter, 1)
    gate_wgrad, up_wgrad, down_grad, stream_part, proj_grad, value_grad, gate_in_grad = mega(
        h_part, rank, weight, w_gate[0], w_up[0], w_down[0], c_part, value, gate_in, normed,
        inv_std[:, None], norm_gain[None, :], taps, w_proj, experts, cap, tp_ways,
    )
    return gate_wgrad[None], up_wgrad[None], down_grad[None], stream_part, proj_grad, value_grad, gate_in_grad


def solution(mesh):
    in_specs = (
        P("sp", None), P("sp", None), P("sp", None), P("sp", None),
        P("sp", None, "tp"), P("sp", None, "tp"), P("sp", "tp", None),
        P("sp", "tp"), P("sp", "tp"), P("sp", "tp"), P("sp"), P("tp"), P(None, "tp"), P(None, "tp"),
    )
    out_specs = (
        P("sp", None, "tp"), P("sp", None, "tp"), P("sp", "tp", None),
        P("sp", "tp"), P("sp", "tp"), P("sp", "tp"), P("sp", "tp"),
    )
    return jax.shard_map(on_device, mesh=mesh, in_specs=in_specs, out_specs=out_specs, check_vma=False)
```
